32 devices in a mesh: grp: 2 (over y), sp: 4 (over z), tp: 4 (over x, core).
Axes of the slice: x: 2, y: 2, z: 4, core: 2. Of those that a mesh axis runs over, the one named last changes fastest.
Arguments:
- tokens_in: bfloat16 [2048, 2048], P(('grp', 'sp')), parts along dimension 0, may hold values from -6 to 6
- input_gain: float32 [2048], replicated, may hold values from 0.1 to 1.9
- w_query: bfloat16 [2048, 1024], P('sp', 'tp'), may hold values from -0.125 to 0.125
- w_key: bfloat16 [2048, 1024], P('sp', 'tp'), may hold values from -1 to 1
- w_value: bfloat16 [2048, 1024], P('sp', 'tp'), may hold values from -0.125 to 0.125
- w_gates: bfloat16 [2048, 32], P('sp', 'tp'), may hold values from -3 to 3
- w_glu_value: bfloat16 [2048, 1024], P('sp', 'tp'), may hold values from -0.125 to 0.125
- sigmoid_opener_matrix: bfloat16 [2048, 1024], P('sp', 'tp'), may hold values from -0.125 to 0.125
- log_decay: float32 [2048, 16], P(('grp', 'sp'), 'tp'), parts along dimension 0, may hold values from -1 to 0
- head_gain: float32 [128], replicated, may hold values from 0.1 to 1.9
- conv_kernel: float32 [31, 1024], P(None, 'tp'), may hold values from -12 to 12
- norm_gain: float32 [1024], P('tp'), may hold values from 0.1 to 1.9
- norm_shift: float32 [1024], P('tp'), may hold values from -3 to 3
- out_delta: bfloat16 [2048, 1024], P(None, 'tp'), may hold values from -0.125 to 0.125
- out_conv: bfloat16 [2048, 1024], P(None, 'tp'), may hold values from -0.125 to 0.125
Outputs:
- mixed: bfloat16 [2048, 2048], P(('grp', 'sp'), 'tp'), parts along dimension 0
The draws below stay inside these ranges and needn't reach their ends.
There are 2 independent parts, one for each index of `grp`. The reference program is written for one: setup_inputs(seed, part) draws one part's arguments, and reference() takes and returns one part's arrays. A program takes and returns all parts, laid end to end along the dimension named above; an argument that names none is the same for every part. Nothing has to cross between parts.
All inputs are finite; a program needn't handle non-finite values.
Results may differ from the reference program's by a relative error of at most 0.015.
Values may be sent and summed in bfloat16 or wider, within the bound.
A program may use at most 64 MiB of HBM per device.

```python
import jax
import jax.numpy as jnp
from jax import lax

D = 2048
HEADS = 8
HEAD_DIM = 128
CONV_CH = 1024
KERNEL = 31
BLOCK = 64
TOK_DEV = 256
SEQ = 1024
A_W = 1024
N_TP = 4


def draw_log_decay(key, part):
    streams = jax.random.split(jax.random.fold_in(key, 11), 6)
    columns = 2 * HEADS
    fast_share = 0.5
    picker = jax.random.uniform(streams[0], (columns,), jnp.float32)
    fast_rate = jax.random.uniform(streams[1], (columns,), jnp.float32, 0.015, 0.04)
    slow_rate = jax.random.uniform(streams[2], (columns,), jnp.float32, 0.04, 0.16) / SEQ
    forgetting_pace = jnp.where(picker < fast_share, fast_rate, slow_rate)
    multiplier_amount = jnp.exp(jax.random.uniform(streams[3], (SEQ // TOK_DEV, columns), jnp.float32, 0.0, 1.0986))
    multiplier_amount = jnp.repeat(multiplier_amount, TOK_DEV, axis=0)
    spots = jax.random.randint(streams[4], (2, columns), 0, SEQ)
    places = jnp.arange(SEQ)[:, None]
    masked_elements = (places == spots[0][None, :]) | (places == spots[1][None, :])
    objective_readings = jax.random.uniform(streams[5], (SEQ, columns), jnp.float32, 0.2, 0.35)
    clustered_bunches = jnp.where(masked_elements, jnp.log(1.0 - objective_readings), 0.0)
    return (-(forgetting_pace[None, :] * multiplier_amount) + clustered_bunches).astype(jnp.float32)


def draw_conv_kernel(key, part):
    streams = jax.random.split(jax.random.fold_in(key, 23), 2)
    channel_slot = jnp.arange(CONV_CH).astype(jnp.float32)
    random_perturbation = jax.random.uniform(streams[1], (CONV_CH,), jnp.float32)
    entries = jnp.clip(jax.random.normal(streams[0], (KERNEL, CONV_CH), jnp.float32), -4.0, 4.0)
    reach = 10.0
    scale = reach ** ((channel_slot + random_perturbation) / CONV_CH)
    return (entries * scale[None, :] / jnp.sqrt(float(KERNEL))).astype(jnp.float32)


def unit_entries(stream, shape):
    return jnp.clip(jax.random.normal(stream, shape, jnp.float32), -4.0, 4.0)


def draw_w_key(key, part):
    streams = jax.random.split(jax.random.fold_in(key, 31), 2)
    strong_count = HEAD_DIM * 3 // 8
    weak_energy = 0.356 * (HEAD_DIM - strong_count)
    ratio_square = max(1.0, (0.04 * SEQ - weak_energy) / (0.5 * strong_count))
    orders = jax.vmap(lambda sub_key: jax.random.permutation(sub_key, HEAD_DIM))(jax.random.split(streams[0], HEADS))
    column_scale = jnp.where(orders < strong_count, ratio_square ** 0.5, 1.0).reshape(HEADS * HEAD_DIM).astype(jnp.float32)
    entries = unit_entries(streams[1], (D, HEADS * HEAD_DIM))
    return (entries * column_scale[None, :] / jnp.sqrt(float(D))).astype(jnp.bfloat16)


def draw_w_gates(key, part):
    stream = jax.random.fold_in(key, 37)
    roles = jnp.arange(4 * HEADS) % 4
    column_scale = jnp.where((roles == 1) | (roles == 3), 4.0, 1.0).astype(jnp.float32)
    entries = unit_entries(stream, (D, 4 * HEADS))
    return (entries * column_scale[None, :] / jnp.sqrt(float(D))).astype(jnp.bfloat16)


def shard_levels(key, extent, shards, smallest, top_value):
    level = 1.0
    for axis_at, parts in shards:
        heights = jax.random.uniform(jax.random.fold_in(jax.random.fold_in(key, 6), axis_at), (parts,), jnp.float32, smallest / len(shards), top_value / len(shards))
        level = level * jnp.repeat(jnp.exp(heights), extent[axis_at] // parts).reshape((-1,) + (1,) * (len(extent) - 1 - axis_at))
    return level


def bell_draw(rng, dims, scale, most, cuts=(), kind=jnp.bfloat16):
    array = jax.random.normal(rng, dims, jnp.float32) * scale
    if len(cuts) > 0:
        array = shard_levels(rng, dims, cuts, -0.22, 0.18) * array
    return jnp.clip(array, min=-most, max=most).astype(kind)


def setup_inputs(seed: int = 0, part: int = 0) -> dict:
    key_list = jax.random.split(jax.random.key(seed), 16)
    part_keys = jax.random.split(jax.random.fold_in(key_list[15], part), 16)
    tokens_in = bell_draw(part_keys[0], (SEQ, D), 1.0, 6.0, ((0, 4),))
    input_gain = jnp.clip(1.0 + 0.18 * jax.random.normal(key_list[1], (D,), jnp.float32), 0.1, 1.9)
    w_query = bell_draw(key_list[2], (D, A_W), D ** -0.5, 0.125, ((0, 4), (1, 4)))
    w_key = draw_w_key(jax.random.fold_in(key_list[15], 71), part)
    w_value = bell_draw(key_list[4], (D, A_W), D ** -0.5, 0.125, ((0, 4), (1, 4)))
    w_gates = draw_w_gates(jax.random.fold_in(key_list[15], 71), part)
    w_glu_value = bell_draw(key_list[6], (D, CONV_CH), D ** -0.5, 0.125, ((0, 4), (1, 4)))
    sigmoid_opener_matrix = bell_draw(key_list[7], (D, CONV_CH), D ** -0.5, 0.125, ((0, 4), (1, 4)))
    log_decay = draw_log_decay(jax.random.fold_in(jax.random.fold_in(key_list[15], part), 71), part)
    head_gain = jnp.clip(1.0 + 0.18 * jax.random.normal(key_list[9], (HEAD_DIM,), jnp.float32), 0.1, 1.9)
    conv_kernel = draw_conv_kernel(jax.random.fold_in(key_list[15], 71), part)
    norm_gain = jnp.clip(1.0 + 0.18 * jax.random.normal(key_list[11], (CONV_CH,), jnp.float32), 0.1, 1.9)
    norm_shift = bell_draw(key_list[12], (CONV_CH,), 0.5, 3.0, ((0, 4),), jnp.float32)
    out_delta = bell_draw(key_list[13], (D, A_W), (A_W + CONV_CH) ** -0.5, 0.125, ((1, 4),))
    out_conv = bell_draw(key_list[14], (D, CONV_CH), (A_W + CONV_CH) ** -0.5, 0.125, ((1, 4),))
    return {"tokens_in": tokens_in, "input_gain": input_gain, "w_query": w_query, "w_key": w_key, "w_value": w_value, "w_gates": w_gates, "w_glu_value": w_glu_value, "sigmoid_opener_matrix": sigmoid_opener_matrix, "log_decay": log_decay, "head_gain": head_gain, "conv_kernel": conv_kernel, "norm_gain": norm_gain, "norm_shift": norm_shift, "out_delta": out_delta, "out_conv": out_conv}


PRECISE = lax.Precision.HIGHEST
EPSILON = 1e-06
BETA_SHIFT = 6.0

def high_dot(left, right):
    return jnp.matmul(left, right, precision=PRECISE)

def swap_last(tensor):
    return jnp.swapaxes(tensor, -1, -2)

def block_terms(query, key_rows, values, decay_log, beta_rate, block):
    head_count, length = (query.shape[0], query.shape[1])
    blocks = length // block

    def to_blocks(tensor):
        return tensor.reshape((head_count, blocks, block) + tensor.shape[2:])
    query, key_rows, values, decay_log, beta_rate = (to_blocks(tensor) for tensor in (query, key_rows, values, decay_log, beta_rate))
    cumulative = jnp.cumsum(decay_log, axis=-1)
    positions = jnp.arange(block)
    on_or_below = positions[:, None] >= positions[None, :]
    strict = positions[:, None] > positions[None, :]
    log_gaps = cumulative[..., :, None] - cumulative[..., None, :]
    weighting = jnp.where(on_or_below, jnp.exp(jnp.where(on_or_below, log_gaps, 0.0)), 0.0)
    scaled_keys = key_rows * beta_rate[..., None]
    lower_part = jnp.where(strict, high_dot(scaled_keys, swap_last(key_rows)) * weighting, 0.0)
    identity = jnp.eye(block, dtype=jnp.float32)
    inverse = jax.scipy.linalg.solve_triangular(identity + lower_part, jnp.broadcast_to(identity, lower_part.shape), lower=True, unit_diagonal=True)
    update = high_dot(inverse, values * beta_rate[..., None])
    mixed_keys = high_dot(inverse, scaled_keys * jnp.exp(cumulative)[..., None])
    in_block = jnp.where(on_or_below, high_dot(query, swap_last(key_rows)) * weighting, 0.0)
    q_decayed = query * jnp.exp(cumulative)[..., None]
    k_decayed = key_rows * jnp.exp(cumulative[..., -1:] - cumulative)[..., None]
    end_decay = jnp.exp(cumulative[..., -1])
    return tuple((jnp.moveaxis(tensor, 1, 0) for tensor in (update, mixed_keys, in_block, q_decayed, k_decayed, end_decay)))

def delta_scan(query, key_rows, values, decay_log, beta_rate):
    stacked = block_terms(query, key_rows, values, decay_log, beta_rate, BLOCK)
    head_count, length, head_width = query.shape

    def advance(state_now, pieces):
        update, mixed_keys, in_block, q_decayed, k_decayed, end_decay = pieces
        new_values = update - high_dot(mixed_keys, state_now)
        output = high_dot(q_decayed, state_now) + high_dot(in_block, new_values)
        state_now = state_now * end_decay[:, None, None] + high_dot(swap_last(k_decayed), new_values)
        return (state_now, output)
    zero_state = jnp.zeros((head_count, head_width, values.shape[2]), jnp.float32)
    _, output = lax.scan(advance, zero_state, stacked)
    return jnp.moveaxis(output, 0, 1).reshape(head_count, length, values.shape[2])

def reference(tokens_in, input_gain, w_query, w_key, w_value, w_gates, w_glu_value, sigmoid_opener_matrix, log_decay, head_gain, conv_kernel, norm_gain, norm_shift, out_delta, out_conv):
    rows = tokens_in.astype(jnp.float32)
    normed = (rows * lax.rsqrt(lax.optimization_barrier(jnp.mean(rows * rows, axis=-1, keepdims=True)) + EPSILON) * input_gain).astype(jnp.bfloat16)

    def project(weight):
        return jnp.dot(normed.astype(jnp.float32), weight.astype(jnp.float32), preferred_element_type=jnp.float32)

    def by_head(tensor):
        return jnp.swapaxes(jax.nn.silu(tensor).reshape(SEQ, HEADS, HEAD_DIM), 0, 1)

    def unit_rows(tensor):
        return tensor * lax.rsqrt(lax.optimization_barrier(jnp.sum(tensor * tensor, axis=-1, keepdims=True)) + EPSILON)
    query = unit_rows(by_head(project(w_query))) * HEAD_DIM ** (-0.5)
    key_rows = unit_rows(by_head(project(w_key)))
    values = by_head(project(w_value))
    gate_parts = project(w_gates).reshape(SEQ, HEADS, 4)
    rate_parts = log_decay.reshape(SEQ, HEADS, 2)
    decay_fore = jnp.swapaxes(rate_parts[:, :, 0] * (0.5 + jax.nn.sigmoid(gate_parts[:, :, 0])), 0, 1)
    beta_fore = jnp.swapaxes(jax.nn.sigmoid(gate_parts[:, :, 1] - BETA_SHIFT), 0, 1)
    decay_back = jnp.swapaxes(rate_parts[:, :, 1] * (0.5 + jax.nn.sigmoid(gate_parts[:, :, 2])), 0, 1)
    beta_back = jnp.swapaxes(jax.nn.sigmoid(gate_parts[:, :, 3] - BETA_SHIFT), 0, 1)

    def reversed_rows(tensor):
        return jnp.flip(tensor, axis=1)
    fore = delta_scan(query, key_rows, values, decay_fore, beta_fore)
    back = reversed_rows(delta_scan(reversed_rows(query), reversed_rows(key_rows), reversed_rows(values), reversed_rows(decay_back), reversed_rows(beta_back)))
    joined = fore + back
    joined = joined * lax.rsqrt(lax.optimization_barrier(jnp.mean(joined * joined, axis=-1, keepdims=True)) + EPSILON) * head_gain
    delta_mix = jnp.swapaxes(joined, 0, 1).reshape(SEQ, HEADS * HEAD_DIM).astype(jnp.bfloat16)
    glu_rows = (project(w_glu_value) * jax.nn.sigmoid(project(sigmoid_opener_matrix))).astype(jnp.bfloat16)
    half_width = KERNEL // 2
    padded = jnp.pad(glu_rows.astype(jnp.float32), ((half_width, half_width), (0, 0)))
    conv_rows = padded[0:SEQ] * conv_kernel[0]
    for offset in range(1, KERNEL):
        conv_rows = conv_rows + padded[offset:offset + SEQ] * conv_kernel[offset]
    center = lax.optimization_barrier(jnp.mean(conv_rows, axis=-1))
    spread = lax.optimization_barrier(jnp.mean(conv_rows * conv_rows, axis=-1)) - center * center
    normal_rows = (conv_rows - center[:, None]) * lax.rsqrt(spread + EPSILON)[:, None]
    filtered_blend = jax.nn.silu(normal_rows * norm_gain + norm_shift).astype(jnp.bfloat16)
    head_cols = HEADS * HEAD_DIM // N_TP
    channel_columns = CONV_CH // N_TP
    result = jnp.zeros((SEQ, D), jnp.float32)
    for group in range(N_TP):
        partial_sum = jnp.dot(delta_mix[:, group * head_cols:(group + 1) * head_cols].astype(jnp.float32), out_delta[:, group * head_cols:(group + 1) * head_cols].T.astype(jnp.float32), preferred_element_type=jnp.float32)
        partial_sum = partial_sum + jnp.dot(filtered_blend[:, group * channel_columns:(group + 1) * channel_columns].astype(jnp.float32), out_conv[:, group * channel_columns:(group + 1) * channel_columns].T.astype(jnp.float32), preferred_element_type=jnp.float32)
        rounded = lax.optimization_barrier(partial_sum.astype(jnp.bfloat16))
        result = result + rounded.astype(jnp.float32)
    return result.astype(jnp.bfloat16)
```

```python
import functools

import jax
import jax.numpy as jnp
from jax import lax
from jax.experimental import pallas as pl
from jax.experimental.pallas import tpu as pltpu
from jax.sharding import PartitionSpec as P

EPSILON = 1e-06
BETA_SHIFT = 6.0
HALO = 16
MESH = pl.DeviceIdType.MESH
F32 = jnp.float32
BF16 = jnp.bfloat16
NT = (((1,), (1,)), ((), ()))
TN = (((0,), (0,)), ((), ()))
NN = (((1,), (0,)), ((), ()))
KEY, GATE, VALUE, QUERY, GLU, OPEN = range(6)


def bdot(left, right, dims=NN):
    return lax.dot_general(
        left.astype(BF16), right.astype(BF16), dims, preferred_element_type=F32
    )


def each(count, action):
    if count <= 8:
        for step in range(count):
            action(step)
    else:
        def body(step, carry):
            action(step)
            return carry

        lax.fori_loop(0, count, body, 0)


def kernel(cfg, tok_h, gain, wk_h, wg_h, wv_h, wq_h, wa_h, wb_h, ld, ldt, hgain, ck, ng, ns, od_h, oc_h,
           out,
           tok, normed, wk, wg, wv, wq, wa, wb, od, oc,
           keys, vals, betas, cums, xinv, gaps, rhs, local_out, reads, maps, ends,
           chain_in, chain_out, glu, halo, pad, conv, stat_out, stat_in, conv_acc, part_out, part_in,
           local_sem, z_send, z_recv, y_send, y_recv, chain_send, chain_recv,
           halo_send, halo_recv, stat_send, stat_recv, part_send, part_recv):
    n_grp, n_sp, n_tp, conv_total = cfg
    grp, sp, tp = lax.axis_index("grp"), lax.axis_index("sp"), lax.axis_index("tp")
    length, width = tok.shape
    rows = wk_h.shape[0]
    channels = wa.shape[1]
    head_width = hgain.shape[1]
    heads = wk.shape[1] // head_width
    share = (rows * 3 // 8) // 16 * 16 if n_grp == 2 else 0
    pulled = rows - share

    sources = (wk_h, wg_h, wv_h, wq_h, wa_h, wb_h)
    targets = (wk, wg, wv, wq, wa, wb)

    def block_of(w, index, start, count):
        if w == GATE:
            return targets[w].at[index]
        return targets[w].at[pl.ds(pl.multiple_of(index * rows + start, 16), count)]

    load_tok = pltpu.make_async_copy(tok_h, tok, local_sem.at[0])
    load_tok.start()
    own = [
        pltpu.make_async_copy(sources[w], block_of(w, sp, 0, rows), local_sem.at[1 + w])
        for w in range(6)
    ]
    for copy in own:
        copy.start()
    load_od = pltpu.make_async_copy(od_h, od, local_sem.at[7])
    load_oc = pltpu.make_async_copy(oc_h, oc, local_sem.at[8])

    barrier = pltpu.get_barrier_semaphore()

    def greet(axis, me, count):
        def one(step):
            pl.semaphore_signal(
                barrier, inc=1, device_id={axis: lax.rem(me + step + 1, count)}, device_id_type=MESH
            )

        each(count - 1, one)

    greet("sp", sp, n_sp)
    greet("tp", tp, n_tp)
    greet("grp", grp, n_grp)
    pl.semaphore_wait(barrier, n_sp + n_tp + n_grp - 3)

    def z_copy(w, step):
        dest = lax.rem(sp + step + 1, n_sp)
        if w == GATE:
            source, target = sources[w], block_of(w, sp, 0, 0)
        else:
            start = pl.multiple_of(grp * share, 16) if share else 0
            source = sources[w].at[pl.ds(start, pulled)]
            target = block_of(w, sp, start, pulled)
        return pltpu.make_async_remote_copy(
            src_ref=source, dst_ref=target,
            send_sem=z_send.at[w, step], recv_sem=z_recv.at[w, step],
            device_id={"sp": dest}, device_id_type=MESH,
        )

    def z_arrival(w, step):
        source = lax.rem(sp + n_sp - step - 1, n_sp)
        if w == GATE:
            place = block_of(w, source, 0, 0)
        else:
            place = block_of(w, source, pl.multiple_of(grp * share, 16) if share else 0, pulled)
        return pltpu.make_async_remote_copy(
            src_ref=place, dst_ref=place,
            send_sem=z_send.at[w, step], recv_sem=z_recv.at[w, step],
            device_id={"sp": source}, device_id_type=MESH,
        )

    def y_copy(w, step):
        source = lax.rem(sp + n_sp - step - 1, n_sp)
        place = block_of(w, source, pl.multiple_of(grp * pulled, 16), share)
        return pltpu.make_async_remote_copy(
            src_ref=place, dst_ref=place,
            send_sem=y_send.at[w, step], recv_sem=y_recv.at[w, step],
            device_id={"grp": 1 - grp}, device_id_type=MESH,
        )

    def y_arrival(w, step):
        source = lax.rem(sp + n_sp - step - 1, n_sp)
        place = block_of(w, source, pl.multiple_of((1 - grp) * pulled, 16), share)
        return pltpu.make_async_remote_copy(
            src_ref=place, dst_ref=place,
            send_sem=y_send.at[w, step], recv_sem=y_recv.at[w, step],
            device_id={"grp": 1 - grp}, device_id_type=MESH,
        )

    for w in range(6):
        each(n_sp - 1, lambda step, w=w: z_copy(w, step).start())

    load_od.start()
    load_oc.start()

    def relay(w):
        def one(step):
            z_arrival(w, step).wait_recv()
            if share and w != GATE:
                y_copy(w, step).start()

        each(n_sp - 1, one)

    def complete(w):
        own[w].wait()
        if share and w != GATE:
            each(n_sp - 1, lambda step: y_arrival(w, step).wait_recv())

    load_tok.wait()
    chunk = 64
    for at in range(0, length, chunk):
        here = tok[at:at + chunk, :].astype(F32)
        scale = lax.rsqrt(jnp.mean(here * here, axis=-1, keepdims=True) + EPSILON)
        normed[at:at + chunk, :] = (here * scale * gain[...]).astype(BF16)

    def project(w):
        return jnp.dot(normed[...], targets[w][...], preferred_element_type=F32)

    def unit_rows(tensor):
        return tensor * lax.rsqrt(jnp.sum(tensor * tensor, axis=-1, keepdims=True) + EPSILON)

    def silu(tensor):
        return tensor * jax.nn.sigmoid(tensor)

    relay(KEY)
    relay(GATE)
    complete(GATE)
    gate_cols = jnp.zeros((length, 4 * heads), F32)
    gate_rows = jnp.zeros((4 * heads, length), F32)
    for index in range(n_sp):
        normed_part = normed[:, index * rows:(index + 1) * rows]
        gate_cols = gate_cols + lax.dot_general(normed_part, wg[index], NT, preferred_element_type=F32)
        gate_rows = gate_rows + lax.dot_general(wg[index], normed_part, NT, preferred_element_type=F32)

    row_at = lax.broadcasted_iota(jnp.int32, (length, length), 0)
    col_at = lax.broadcasted_iota(jnp.int32, (length, length), 1)

    complete(KEY)
    key_proj = silu(project(KEY))
    pairs = [(h, r) for h in range(heads) for r in range(2)]
    for h in range(heads):
        keys[h] = unit_rows(key_proj[:, h * head_width:(h + 1) * head_width])
    lowers = [None] * len(pairs)
    for h in range(heads):
        grams = bdot(keys[h], keys[h], NT)
        for r in range(2):
            p = 2 * h + r
            decay_col = ld[:, p:p + 1] * (0.5 + jax.nn.sigmoid(gate_cols[:, 2 * p:2 * p + 1]))
            decay_row = ldt[p:p + 1, :] * (0.5 + jax.nn.sigmoid(gate_rows[2 * p:2 * p + 1, :]))
            beta = jax.nn.sigmoid(gate_cols[:, 2 * p + 1:2 * p + 2] - BETA_SHIFT)
            if r == 0:
                seen_down, seen_across = row_at <= col_at, col_at <= row_at
            else:
                seen_down, seen_across = row_at >= col_at, col_at >= row_at
            cum_row = jnp.sum(jnp.where(seen_down, decay_col, 0.0), axis=0, keepdims=True)
            cum_col = jnp.sum(jnp.where(seen_across, decay_row, 0.0), axis=1, keepdims=True)
            weighting = jnp.where(
                seen_across, jnp.exp(jnp.where(seen_across, cum_col - cum_row, 0.0)), 0.0
            )
            gaps[p] = weighting
            betas[p] = jnp.broadcast_to(beta, (length, head_width))
            cums[p] = jnp.broadcast_to(cum_col, (length, head_width))
            lower = jnp.where(row_at != col_at, grams * weighting * beta, 0.0)
            rhs[p] = lower
            near = (row_at // 2 == col_at // 2)
            xinv[p] = jnp.where(row_at == col_at, 1.0, jnp.where(near, -lower, 0.0))

    size = 2
    while size < length:
        inside = (row_at // (2 * size) == col_at // (2 * size)) & (row_at // size != col_at // size)
        for p in range(len(pairs)):
            across = jnp.where(inside, rhs[p], 0.0)
            inverse = xinv[p]
            xinv[p] = inverse - bdot(inverse, bdot(across, inverse))
        if size == 8:
            relay(VALUE)
        size *= 2

    complete(VALUE)
    value_proj = silu(project(VALUE))
    eye = (
        lax.broadcasted_iota(jnp.int32, (head_width, head_width), 0)
        == lax.broadcasted_iota(jnp.int32, (head_width, head_width), 1)
    )
    for h, r in pairs:
        p = 2 * h + r
        beta, cum, key = betas[p], cums[p], keys[h]
        value = value_proj[:, h * head_width:(h + 1) * head_width]
        total = cum[length - 1:length, :] if r == 0 else cum[0:1, :]
        right = jnp.concatenate([beta * value, beta * key * jnp.exp(cum)], axis=1)
        solved = bdot(xinv[p], right)
        vals[p] = solved.astype(BF16)
        passed = bdot(key * jnp.exp(total - cum), solved, TN)
        ends[p] = passed[:, :head_width]
        maps[p] = (jnp.where(eye, jnp.exp(total), 0.0) - passed[:, head_width:]).astype(BF16)

    def place_of(r):
        return sp if r == 0 else n_sp - 1 - sp

    def chain_copy(r):
        dest = lax.rem(sp + 1, n_sp) if r == 0 else lax.rem(sp + n_sp - 1, n_sp)
        return pltpu.make_async_remote_copy(
            src_ref=chain_out.at[r], dst_ref=chain_in.at[r],
            send_sem=chain_send.at[r], recv_sem=chain_recv.at[r],
            device_id={"sp": dest}, device_id_type=MESH,
        )

    def chain_point(low, high):
        for r in range(2):
            at = place_of(r)

            @pl.when((at >= low) & (at <= high))
            def _(r=r, at=at):
                if low == 0:
                    for h in range(heads):
                        chain_in[r, h] = jnp.zeros((head_width, head_width), BF16)
                        chain_out[r, h] = ends[2 * h + r].astype(BF16)
                else:
                    chain_copy(r).wait_recv()
                    for h in range(heads):
                        p = 2 * h + r
                        chain_out[r, h] = (bdot(maps[p], chain_in[r, h]) + ends[p]).astype(BF16)

                @pl.when(at < n_sp - 1)
                def _():
                    chain_copy(r).start()

    chain_point(0, 0)
    relay(QUERY)
    complete(QUERY)
    query_proj = silu(project(QUERY))
    for h in range(heads):
        query = unit_rows(query_proj[:, h * head_width:(h + 1) * head_width]) * head_width ** -0.5
        scores = bdot(query, keys[h], NT)
        for r in range(2):
            p = 2 * h + r
            both = jnp.dot((scores * gaps[p]).astype(BF16), vals[p], preferred_element_type=F32)
            reads[p] = (query * jnp.exp(cums[p]) - both[:, head_width:]).astype(BF16)
            if r == 0:
                local_out[h] = both[:, :head_width]
            else:
                local_out[h] = local_out[h] + both[:, :head_width]
    chain_point(1, 1)
    relay(GLU)
    chain_point(2, 2)
    relay(OPEN)
    complete(GLU)
    glu_proj = project(GLU)
    chain_point(3, n_sp - 1)
    complete(OPEN)
    gated = (glu_proj * jax.nn.sigmoid(project(OPEN))).astype(BF16)
    glu[...] = gated
    pad[HALO:HALO + length, :] = gated.astype(F32)

    def halo_copy(r):
        start = length - HALO if r == 0 else 0
        dest = lax.rem(sp + 1, n_sp) if r == 0 else lax.rem(sp + n_sp - 1, n_sp)
        return pltpu.make_async_remote_copy(
            src_ref=glu.at[pl.ds(start, HALO)], dst_ref=halo.at[r],
            send_sem=halo_send.at[r], recv_sem=halo_recv.at[r],
            device_id={"sp": dest}, device_id_type=MESH,
        )

    for r in range(2):
        @pl.when(place_of(r) < n_sp - 1)
        def _(r=r):
            halo_copy(r).start()
    for r in range(2):
        start = 0 if r == 0 else HALO + length

        @pl.when(place_of(r) > 0)
        def _(r=r, start=start):
            halo_copy(r).wait_recv()
            pad[start:start + HALO, :] = halo[r].astype(F32)

        @pl.when(place_of(r) == 0)
        def _(start=start):
            pad[start:start + HALO, :] = jnp.zeros((HALO, channels), F32)

    taps = ck.shape[0]
    for at in range(0, length, chunk):
        first = at + HALO - taps // 2
        total = pad[first:first + chunk, :] * ck[0:1, :]
        for j in range(1, taps):
            total = total + pad[first + j:first + j + chunk, :] * ck[j:j + 1, :]
        conv[at:at + chunk, :] = total
    filtered = conv[...]
    sum_col = jnp.sum(filtered, axis=-1, keepdims=True)
    square_col = jnp.sum(filtered * filtered, axis=-1, keepdims=True)
    same = row_at == col_at
    stat_out[...] = jnp.zeros(stat_out.shape, F32)
    stat_out[0:1, :] = jnp.sum(jnp.where(same, sum_col, 0.0), axis=0, keepdims=True)
    stat_out[1:2, :] = jnp.sum(jnp.where(same, square_col, 0.0), axis=0, keepdims=True)

    def stat_copy(step):
        return pltpu.make_async_remote_copy(
            src_ref=stat_out, dst_ref=stat_in.at[step],
            send_sem=stat_send.at[step], recv_sem=stat_recv.at[step],
            device_id={"tp": lax.rem(tp + step + 1, n_tp)}, device_id_type=MESH,
        )

    for step in range(n_tp - 1):
        stat_copy(step).start()

    joined_heads = []
    for h in range(heads):
        joined = local_out[h] + jnp.dot(reads[2 * h], chain_in[0, h], preferred_element_type=F32)
        joined = joined + jnp.dot(reads[2 * h + 1], chain_in[1, h], preferred_element_type=F32)
        scale = lax.rsqrt(jnp.mean(joined * joined, axis=-1, keepdims=True) + EPSILON)
        joined_heads.append((joined * scale * hgain[...]).astype(BF16))
    delta_mix = jnp.concatenate(joined_heads, axis=1) if heads > 1 else joined_heads[0]
    load_od.wait()
    load_oc.wait()
    columns = width // n_tp
    order = [(step + n_tp // 2) % n_tp for step in range(n_tp)]
    order = [o for o in order if o] + [0]

    def rows_of(matrix, o):
        dest = lax.rem(tp + o, n_tp)
        return matrix[pl.ds(pl.multiple_of(dest * columns, 16), columns), :]

    for o in order:
        conv_acc[o] = lax.dot_general(delta_mix, rows_of(od, o), NT, preferred_element_type=F32)

    stats = stat_out[0:2, :]
    for step in range(n_tp - 1):
        stat_copy(step).wait_recv()
        stats = stats + stat_in[step, 0:2, :]
    center = jnp.sum(jnp.where(same, stats[0:1, :], 0.0), axis=1, keepdims=True) / conv_total
    squares = jnp.sum(jnp.where(same, stats[1:2, :], 0.0), axis=1, keepdims=True) / conv_total
    spread = squares - center * center
    normal = (filtered - center) * lax.rsqrt(spread + EPSILON)
    conv_mix = silu(normal * ng[...] + ns[...]).astype(BF16)

    def part_copy(o):
        return pltpu.make_async_remote_copy(
            src_ref=part_out.at[o - 1], dst_ref=part_in.at[o - 1],
            send_sem=part_send.at[o - 1], recv_sem=part_recv.at[o - 1],
            device_id={"tp": lax.rem(tp + o, n_tp)}, device_id_type=MESH,
        )

    for o in order:
        term = conv_acc[o] + lax.dot_general(conv_mix, rows_of(oc, o), NT, preferred_element_type=F32)
        if o:
            part_out[o - 1] = term.astype(BF16)
            part_copy(o).start()
        else:
            result = term.astype(BF16).astype(F32)
    for o in range(1, n_tp):
        part_copy(o).wait_recv()
        result = result + part_in[o - 1].astype(F32)
    out[...] = result.astype(BF16)

    for w in range(6):
        each(n_sp - 1, lambda step, w=w: z_copy(w, step).wait_send())
        if share and w != GATE:
            each(n_sp - 1, lambda step, w=w: y_copy(w, step).wait_send())
    for r in range(2):
        @pl.when(place_of(r) < n_sp - 1)
        def _(r=r):
            chain_copy(r).wait_send()
            halo_copy(r).wait_send()
    for step in range(n_tp - 1):
        stat_copy(step).wait_send()
        part_copy(step + 1).wait_send()


def solution(mesh):
    n_grp, n_sp, n_tp = mesh.shape["grp"], mesh.shape["sp"], mesh.shape["tp"]

    def on_device(tokens_in, input_gain, w_query, w_key, w_value, w_gates, w_glu_value,
                  sigmoid_opener_matrix, log_decay, head_gain, conv_kernel, norm_gain, norm_shift,
                  out_delta, out_conv):
        length, width = tokens_in.shape
        head_width = head_gain.shape[0]
        head_cols = w_query.shape[1]
        heads = head_cols // head_width
        channels = w_glu_value.shape[1]
        rows = w_query.shape[0]
        pairs = 2 * heads
        columns = width // n_tp
        dma, vmem = pltpu.SemaphoreType.DMA, pltpu.VMEM
        anywhere = pl.BlockSpec(memory_space=pltpu.HBM)
        inside = pl.BlockSpec(memory_space=pltpu.VMEM)
        scratch = [
            vmem((length, width), BF16), vmem((length, width), BF16),
            vmem((width, head_cols), BF16), vmem((n_sp, 4 * heads, rows), BF16),
            vmem((width, head_cols), BF16), vmem((width, head_cols), BF16),
            vmem((width, channels), BF16), vmem((width, channels), BF16),
            vmem((width, head_cols), BF16), vmem((width, channels), BF16),
            vmem((heads, length, head_width), F32), vmem((pairs, length, 2 * head_width), BF16),
            vmem((pairs, length, head_width), F32), vmem((pairs, length, head_width), F32),
            vmem((pairs, length, length), F32), vmem((pairs, length, length), F32),
            vmem((pairs, length, length), F32),
            vmem((heads, length, head_width), F32), vmem((pairs, length, head_width), BF16),
            vmem((pairs, head_width, head_width), BF16), vmem((pairs, head_width, head_width), F32),
            vmem((2, heads, head_width, head_width), BF16), vmem((2, heads, head_width, head_width), BF16),
            vmem((length, channels), BF16), vmem((2, HALO, channels), BF16),
            vmem((length + 2 * HALO, channels), F32), vmem((length, channels), F32),
            vmem((8, length), F32), vmem((n_tp - 1, 8, length), F32),
            vmem((n_tp, length, columns), F32),
            vmem((n_tp - 1, length, columns), BF16), vmem((n_tp - 1, length, columns), BF16),
            dma((9,)),
            dma((6, n_sp - 1)), dma((6, n_sp - 1)), dma((6, n_sp - 1)), dma((6, n_sp - 1)),
            dma((2,)), dma((2,)), dma((2,)), dma((2,)),
            dma((n_tp - 1,)), dma((n_tp - 1,)), dma((n_tp - 1,)), dma((n_tp - 1,)),
        ]
        return pl.pallas_call(
            functools.partial(kernel, (n_grp, n_sp, n_tp, float(channels * n_tp))),
            out_shape=jax.ShapeDtypeStruct((length, columns), BF16),
            in_specs=[anywhere, inside] + [anywhere] * 6 + [inside] * 6 + [anywhere] * 2,
            out_specs=inside,
            scratch_shapes=scratch,
            compiler_params=pltpu.CompilerParams(
                collective_id=0, has_side_effects=True, vmem_limit_bytes=60 * 1024 * 1024
            ),
        )(
            tokens_in, input_gain.reshape(1, width), w_key, w_gates.T, w_value, w_query,
            w_glu_value, sigmoid_opener_matrix, log_decay, log_decay.T,
            head_gain.reshape(1, head_width), conv_kernel, norm_gain.reshape(1, channels),
            norm_shift.reshape(1, channels), out_delta, out_conv,
        )

    placed = (
        P(("grp", "sp"), None), P(), P("sp", "tp"), P("sp", "tp"), P("sp", "tp"), P("sp", "tp"),
        P("sp", "tp"), P("sp", "tp"), P(("grp", "sp"), "tp"), P(), P(None, "tp"), P("tp"), P("tp"),
        P(None, "tp"), P(None, "tp"),
    )
    return jax.shard_map(
        on_device, mesh=mesh, in_specs=placed, out_specs=P(("grp", "sp"), "tp"), check_vma=False
    )
```

```python
import functools

import jax
import jax.numpy as jnp
from jax import lax
from jax.experimental import pallas as pl
from jax.experimental.pallas import tpu as pltpu
from jax.sharding import PartitionSpec as P

EPSILON = 1e-06
BETA_SHIFT = 6.0
HALO = 16
MESH = pl.DeviceIdType.MESH
F32 = jnp.float32
BF16 = jnp.bfloat16
NT = (((1,), (1,)), ((), ()))
TN = (((0,), (0,)), ((), ()))
NN = (((1,), (0,)), ((), ()))
KEY, GATE, VALUE, QUERY, GLU, OPEN = range(6)


def bdot(left, right, dims=NN):
    return lax.dot_general(
        left.astype(BF16), right.astype(BF16), dims, preferred_element_type=F32
    )


def each(count, action):
    if count <= 8:
        for step in range(count):
            action(step)
    else:
        def body(step, carry):
            action(step)
            return carry

        lax.fori_loop(0, count, body, 0)


def kernel(cfg, tok_h, gain, wk_h, wg_h, wv_h, wq_h, wa_h, wb_h, ld, ldt, hgain, ck, ng, ns, od_h, oc_h,
           out,
           tok, normed, wk, wg, wv, wq, wa, wb, od, oc,
           keys, vals, betas, cums, xinv, gaps, rhs, local_out, reads, maps, ends,
           chain_in, chain_out, glu, halo, pad, conv, stat_out, stat_in, conv_acc, part_out, part_in,
           local_sem, z_send, z_recv, y_send, y_recv, chain_send, chain_recv,
           halo_send, halo_recv, stat_send, stat_recv, part_send, part_recv):
    n_grp, n_sp, n_tp, conv_total = cfg
    grp, sp, tp = lax.axis_index("grp"), lax.axis_index("sp"), lax.axis_index("tp")
    length, width = tok.shape
    rows = wk_h.shape[0]
    channels = wa.shape[1]
    head_width = hgain.shape[1]
    heads = wk.shape[1] // head_width
    share = (rows // 2) // 16 * 16 if n_grp == 2 else 0
    pulled = rows - share

    sources = (wk_h, wg_h, wv_h, wq_h, wa_h, wb_h)
    targets = (wk, wg, wv, wq, wa, wb)

    def block_of(w, index, start, count):
        if w == GATE:
            return targets[w].at[index]
        return targets[w].at[pl.ds(pl.multiple_of(index * rows + start, 16), count)]

    load_tok = pltpu.make_async_copy(tok_h, tok, local_sem.at[0])
    load_tok.start()
    own = [
        pltpu.make_async_copy(sources[w], block_of(w, sp, 0, rows), local_sem.at[1 + w])
        for w in range(6)
    ]
    for copy in own:
        copy.start()
    load_od = pltpu.make_async_copy(od_h, od, local_sem.at[7])
    load_oc = pltpu.make_async_copy(oc_h, oc, local_sem.at[8])

    barrier = pltpu.get_barrier_semaphore()

    def greet(axis, me, count):
        def one(step):
            pl.semaphore_signal(
                barrier, inc=1, device_id={axis: lax.rem(me + step + 1, count)}, device_id_type=MESH
            )

        each(count - 1, one)

    greet("sp", sp, n_sp)
    greet("tp", tp, n_tp)
    greet("grp", grp, n_grp)
    pl.semaphore_wait(barrier, n_sp + n_tp + n_grp - 3)

    def origin(side, d):
        return sp - d if side == 0 else sp + d

    def arrives(side, d):
        return sp - d >= 0 if side == 0 else sp + d < n_sp

    def leaves(side, d):
        if side == 0:
            return (sp - (d - 1) >= 0) & (sp < n_sp - 1)
        return (sp + (d - 1) < n_sp) & (sp > 0)

    def part_of(w, index, side_of):
        if w == GATE:
            return block_of(w, index, 0, 0)
        if not share:
            return block_of(w, index, 0, rows)
        if side_of is None:
            return block_of(w, index, pl.multiple_of(grp * share, 16), pulled)
        return block_of(w, index, pl.multiple_of(side_of * pulled, 16), share)

    def z_copy(w, side, d, first=False):
        target = part_of(w, origin(side, d - 1), None)
        source = target
        if first:
            source = sources[w]
            if w != GATE and share:
                source = source.at[pl.ds(pl.multiple_of(grp * share, 16), pulled)]
        return pltpu.make_async_remote_copy(
            src_ref=source, dst_ref=target,
            send_sem=z_send.at[w, side, d - 1], recv_sem=z_recv.at[w, side, d - 1],
            device_id={"sp": sp + 1 if side == 0 else sp - 1}, device_id_type=MESH,
        )

    def z_arrival(w, side, d):
        place = part_of(w, origin(side, d), None)
        return pltpu.make_async_remote_copy(
            src_ref=place, dst_ref=place,
            send_sem=z_send.at[w, side, d - 1], recv_sem=z_recv.at[w, side, d - 1],
            device_id={"sp": sp + 1 if side == 0 else sp - 1}, device_id_type=MESH,
        )

    def y_copy(w, side, d, arriving=False):
        place = part_of(w, origin(side, d), 1 - grp if arriving else grp)
        return pltpu.make_async_remote_copy(
            src_ref=place, dst_ref=place,
            send_sem=y_send.at[w, side, d - 1], recv_sem=y_recv.at[w, side, d - 1],
            device_id={"grp": 1 - grp}, device_id_type=MESH,
        )

    def offer(w):
        for side in range(2):
            @pl.when(leaves(side, 1))
            def _(side=side):
                z_copy(w, side, 1, True).start()

    def relay_hop(w, d):
        for side in range(2):
            @pl.when(arrives(side, d))
            def _(side=side):
                z_arrival(w, side, d).wait_recv()

                @pl.when(leaves(side, d + 1))
                def _():
                    z_copy(w, side, d + 1).start()

                if share and w != GATE:
                    y_copy(w, side, d).start()

    def relay(w, low=1, high=None):
        if high is None:
            each(n_sp - low, lambda step: relay_hop(w, step + low))
        else:
            for d in range(low, min(high, n_sp - 1) + 1):
                relay_hop(w, d)

    def complete(w):
        own[w].wait()
        if share and w != GATE:
            def one(step):
                for side in range(2):
                    @pl.when(arrives(side, step + 1))
                    def _(side=side):
                        y_copy(w, side, step + 1, True).wait_recv()

            each(n_sp - 1, one)

    offer(KEY)
    offer(GATE)
    offer(VALUE)
    load_od.start()
    load_oc.start()

    load_tok.wait()
    chunk = 64
    for at in range(0, length, chunk):
        here = tok[at:at + chunk, :].astype(F32)
        scale = lax.rsqrt(jnp.mean(here * here, axis=-1, keepdims=True) + EPSILON)
        normed[at:at + chunk, :] = (here * scale * gain[...]).astype(BF16)

    def project(w):
        return jnp.dot(normed[...], targets[w][...], preferred_element_type=F32)

    def unit_rows(tensor):
        return tensor * lax.rsqrt(jnp.sum(tensor * tensor, axis=-1, keepdims=True) + EPSILON)

    def silu(tensor):
        return tensor * jax.nn.sigmoid(tensor)

    relay(GATE)
    relay(KEY)
    offer(QUERY)
    complete(GATE)
    gate_cols = jnp.zeros((length, 4 * heads), F32)
    gate_rows = jnp.zeros((4 * heads, length), F32)
    for index in range(n_sp):
        normed_part = normed[:, index * rows:(index + 1) * rows]
        gate_cols = gate_cols + lax.dot_general(normed_part, wg[index], NT, preferred_element_type=F32)
        gate_rows = gate_rows + lax.dot_general(wg[index], normed_part, NT, preferred_element_type=F32)

    row_at = lax.broadcasted_iota(jnp.int32, (length, length), 0)
    col_at = lax.broadcasted_iota(jnp.int32, (length, length), 1)

    complete(KEY)
    key_proj = silu(project(KEY))
    pairs = [(h, r) for h in range(heads) for r in range(2)]
    for h in range(heads):
        keys[h] = unit_rows(key_proj[:, h * head_width:(h + 1) * head_width])
    relay(VALUE, 1, 1)
    for h in range(heads):
        grams = bdot(keys[h], keys[h], NT)
        for r in range(2):
            p = 2 * h + r
            decay_col = ld[:, p:p + 1] * (0.5 + jax.nn.sigmoid(gate_cols[:, 2 * p:2 * p + 1]))
            decay_row = ldt[p:p + 1, :] * (0.5 + jax.nn.sigmoid(gate_rows[2 * p:2 * p + 1, :]))
            beta = jax.nn.sigmoid(gate_cols[:, 2 * p + 1:2 * p + 2] - BETA_SHIFT)
            if r == 0:
                seen_down, seen_across = row_at <= col_at, col_at <= row_at
            else:
                seen_down, seen_across = row_at >= col_at, col_at >= row_at
            cum_row = jnp.sum(jnp.where(seen_down, decay_col, 0.0), axis=0, keepdims=True)
            cum_col = jnp.sum(jnp.where(seen_across, decay_row, 0.0), axis=1, keepdims=True)
            weighting = jnp.where(
                seen_across, jnp.exp(jnp.where(seen_across, cum_col - cum_row, 0.0)), 0.0
            )
            gaps[p] = weighting
            betas[p] = jnp.broadcast_to(beta, (length, head_width))
            cums[p] = jnp.broadcast_to(cum_col, (length, head_width))
            lower = jnp.where(row_at != col_at, grams * weighting * beta, 0.0)
            rhs[p] = lower
            near = (row_at // 2 == col_at // 2)
            xinv[p] = jnp.where(row_at == col_at, 1.0, jnp.where(near, -lower, 0.0))

    size = 2
    while size < length:
        inside = (row_at // (2 * size) == col_at // (2 * size)) & (row_at // size != col_at // size)
        for p in range(len(pairs)):
            across = jnp.where(inside, rhs[p], 0.0)
            inverse = xinv[p]
            xinv[p] = inverse - bdot(inverse, bdot(across, inverse))
        if size == 2:
            relay(VALUE, 2)
            offer(GLU)
        if size == 32:
            relay(QUERY, 1, 1)
        if size == 128:
            relay(QUERY, 2, 2)
        size *= 2

    complete(VALUE)
    value_proj = silu(project(VALUE))
    eye = (
        lax.broadcasted_iota(jnp.int32, (head_width, head_width), 0)
        == lax.broadcasted_iota(jnp.int32, (head_width, head_width), 1)
    )
    for h, r in pairs:
        p = 2 * h + r
        beta, cum, key = betas[p], cums[p], keys[h]
        value = value_proj[:, h * head_width:(h + 1) * head_width]
        total = cum[length - 1:length, :] if r == 0 else cum[0:1, :]
        right = jnp.concatenate([beta * value, beta * key * jnp.exp(cum)], axis=1)
        solved = bdot(xinv[p], right)
        vals[p] = solved.astype(BF16)
        passed = bdot(key * jnp.exp(total - cum), solved, TN)
        ends[p] = passed[:, :head_width]
        maps[p] = (jnp.where(eye, jnp.exp(total), 0.0) - passed[:, head_width:]).astype(BF16)

    def place_of(r):
        return sp if r == 0 else n_sp - 1 - sp

    def chain_copy(r):
        dest = lax.rem(sp + 1, n_sp) if r == 0 else lax.rem(sp + n_sp - 1, n_sp)
        return pltpu.make_async_remote_copy(
            src_ref=chain_out.at[r], dst_ref=chain_in.at[r],
            send_sem=chain_send.at[r], recv_sem=chain_recv.at[r],
            device_id={"sp": dest}, device_id_type=MESH,
        )

    def chain_point(low, high):
        for r in range(2):
            at = place_of(r)

            @pl.when((at >= low) & (at <= high))
            def _(r=r, at=at):
                if low == 0:
                    for h in range(heads):
                        chain_in[r, h] = jnp.zeros((head_width, head_width), BF16)
                        chain_out[r, h] = ends[2 * h + r].astype(BF16)
                else:
                    chain_copy(r).wait_recv()
                    for h in range(heads):
                        p = 2 * h + r
                        chain_out[r, h] = (bdot(maps[p], chain_in[r, h]) + ends[p]).astype(BF16)

                @pl.when(at < n_sp - 1)
                def _():
                    chain_copy(r).start()

    chain_point(0, 0)
    relay(QUERY, 3)
    offer(OPEN)
    relay(GLU, 1, 1)
    complete(QUERY)
    query_proj = silu(project(QUERY))
    for h in range(heads):
        query = unit_rows(query_proj[:, h * head_width:(h + 1) * head_width]) * head_width ** -0.5
        scores = bdot(query, keys[h], NT)
        for r in range(2):
            p = 2 * h + r
            both = jnp.dot((scores * gaps[p]).astype(BF16), vals[p], preferred_element_type=F32)
            reads[p] = (query * jnp.exp(cums[p]) - both[:, head_width:]).astype(BF16)
            if r == 0:
                local_out[h] = both[:, :head_width]
            else:
                local_out[h] = local_out[h] + both[:, :head_width]
    chain_point(1, 1)
    relay(GLU, 2, 2)
    chain_point(2, 2)
    relay(GLU, 3)
    relay(OPEN, 1, 1)
    chain_point(3, n_sp - 1)
    complete(GLU)
    glu_proj = project(GLU)
    relay(OPEN, 2)
    complete(OPEN)
    gated = (glu_proj * jax.nn.sigmoid(project(OPEN))).astype(BF16)
    glu[...] = gated
    pad[HALO:HALO + length, :] = gated.astype(F32)

    def halo_copy(r):
        start = length - HALO if r == 0 else 0
        dest = lax.rem(sp + 1, n_sp) if r == 0 else lax.rem(sp + n_sp - 1, n_sp)
        return pltpu.make_async_remote_copy(
            src_ref=glu.at[pl.ds(start, HALO)], dst_ref=halo.at[r],
            send_sem=halo_send.at[r], recv_sem=halo_recv.at[r],
            device_id={"sp": dest}, device_id_type=MESH,
        )

    for r in range(2):
        @pl.when(place_of(r) < n_sp - 1)
        def _(r=r):
            halo_copy(r).start()
    for r in range(2):
        start = 0 if r == 0 else HALO + length

        @pl.when(place_of(r) > 0)
        def _(r=r, start=start):
            halo_copy(r).wait_recv()
            pad[start:start + HALO, :] = halo[r].astype(F32)

        @pl.when(place_of(r) == 0)
        def _(start=start):
            pad[start:start + HALO, :] = jnp.zeros((HALO, channels), F32)

    taps = ck.shape[0]
    for at in range(0, length, chunk):
        first = at + HALO - taps // 2
        total = pad[first:first + chunk, :] * ck[0:1, :]
        for j in range(1, taps):
            total = total + pad[first + j:first + j + chunk, :] * ck[j:j + 1, :]
        conv[at:at + chunk, :] = total
    filtered = conv[...]
    sum_col = jnp.sum(filtered, axis=-1, keepdims=True)
    square_col = jnp.sum(filtered * filtered, axis=-1, keepdims=True)
    same = row_at == col_at
    stat_out[...] = jnp.zeros(stat_out.shape, F32)
    stat_out[0:1, :] = jnp.sum(jnp.where(same, sum_col, 0.0), axis=0, keepdims=True)
    stat_out[1:2, :] = jnp.sum(jnp.where(same, square_col, 0.0), axis=0, keepdims=True)

    def stat_copy(step):
        return pltpu.make_async_remote_copy(
            src_ref=stat_out, dst_ref=stat_in.at[step],
            send_sem=stat_send.at[step], recv_sem=stat_recv.at[step],
            device_id={"tp": lax.rem(tp + step + 1, n_tp)}, device_id_type=MESH,
        )

    for step in range(n_tp - 1):
        stat_copy(step).start()

    joined_heads = []
    for h in range(heads):
        joined = local_out[h] + jnp.dot(reads[2 * h], chain_in[0, h], preferred_element_type=F32)
        joined = joined + jnp.dot(reads[2 * h + 1], chain_in[1, h], preferred_element_type=F32)
        scale = lax.rsqrt(jnp.mean(joined * joined, axis=-1, keepdims=True) + EPSILON)
        joined_heads.append((joined * scale * hgain[...]).astype(BF16))
    delta_mix = jnp.concatenate(joined_heads, axis=1) if heads > 1 else joined_heads[0]
    load_od.wait()
    load_oc.wait()
    columns = width // n_tp
    order = [(step + n_tp // 2) % n_tp for step in range(n_tp)]
    order = [o for o in order if o] + [0]

    def rows_of(matrix, o):
        dest = lax.rem(tp + o, n_tp)
        return matrix[pl.ds(pl.multiple_of(dest * columns, 16), columns), :]

    for o in order:
        conv_acc[o] = lax.dot_general(delta_mix, rows_of(od, o), NT, preferred_element_type=F32)

    stats = stat_out[0:2, :]
    for step in range(n_tp - 1):
        stat_copy(step).wait_recv()
        stats = stats + stat_in[step, 0:2, :]
    center = jnp.sum(jnp.where(same, stats[0:1, :], 0.0), axis=1, keepdims=True) / conv_total
    squares = jnp.sum(jnp.where(same, stats[1:2, :], 0.0), axis=1, keepdims=True) / conv_total
    spread = squares - center * center
    normal = (filtered - center) * lax.rsqrt(spread + EPSILON)
    conv_mix = silu(normal * ng[...] + ns[...]).astype(BF16)

    def part_copy(o):
        return pltpu.make_async_remote_copy(
            src_ref=part_out.at[o - 1], dst_ref=part_in.at[o - 1],
            send_sem=part_send.at[o - 1], recv_sem=part_recv.at[o - 1],
            device_id={"tp": lax.rem(tp + o, n_tp)}, device_id_type=MESH,
        )

    for o in order:
        term = conv_acc[o] + lax.dot_general(conv_mix, rows_of(oc, o), NT, preferred_element_type=F32)
        if o:
            part_out[o - 1] = term.astype(BF16)
            part_copy(o).start()
        else:
            result = term.astype(BF16).astype(F32)
    for o in range(1, n_tp):
        part_copy(o).wait_recv()
        result = result + part_in[o - 1].astype(F32)
    out[...] = result.astype(BF16)

    for w in range(6):
        def one(step, w=w):
            for side in range(2):
                @pl.when(leaves(side, step + 1))
                def _(side=side):
                    z_copy(w, side, step + 1).wait_send()

                if share and w != GATE:
                    @pl.when(arrives(side, step + 1))
                    def _(side=side):
                        y_copy(w, side, step + 1).wait_send()

        each(n_sp - 1, one)
    for r in range(2):
        @pl.when(place_of(r) < n_sp - 1)
        def _(r=r):
            chain_copy(r).wait_send()
            halo_copy(r).wait_send()
    for step in range(n_tp - 1):
        stat_copy(step).wait_send()
        part_copy(step + 1).wait_send()


def solution(mesh):
    n_grp, n_sp, n_tp = mesh.shape["grp"], mesh.shape["sp"], mesh.shape["tp"]

    def on_device(tokens_in, input_gain, w_query, w_key, w_value, w_gates, w_glu_value,
                  sigmoid_opener_matrix, log_decay, head_gain, conv_kernel, norm_gain, norm_shift,
                  out_delta, out_conv):
        length, width = tokens_in.shape
        head_width = head_gain.shape[0]
        head_cols = w_query.shape[1]
        heads = head_cols // head_width
        channels = w_glu_value.shape[1]
        rows = w_query.shape[0]
        pairs = 2 * heads
        columns = width // n_tp
        dma, vmem = pltpu.SemaphoreType.DMA, pltpu.VMEM
        anywhere = pl.BlockSpec(memory_space=pltpu.HBM)
        inside = pl.BlockSpec(memory_space=pltpu.VMEM)
        scratch = [
            vmem((length, width), BF16), vmem((length, width), BF16),
            vmem((width, head_cols), BF16), vmem((n_sp, 4 * heads, rows), BF16),
            vmem((width, head_cols), BF16), vmem((width, head_cols), BF16),
            vmem((width, channels), BF16), vmem((width, channels), BF16),
            vmem((width, head_cols), BF16), vmem((width, channels), BF16),
            vmem((heads, length, head_width), F32), vmem((pairs, length, 2 * head_width), BF16),
            vmem((pairs, length, head_width), F32), vmem((pairs, length, head_width), F32),
            vmem((pairs, length, length), F32), vmem((pairs, length, length), F32),
            vmem((pairs, length, length), F32),
            vmem((heads, length, head_width), F32), vmem((pairs, length, head_width), BF16),
            vmem((pairs, head_width, head_width), BF16), vmem((pairs, head_width, head_width), F32),
            vmem((2, heads, head_width, head_width), BF16), vmem((2, heads, head_width, head_width), BF16),
            vmem((length, channels), BF16), vmem((2, HALO, channels), BF16),
            vmem((length + 2 * HALO, channels), F32), vmem((length, channels), F32),
            vmem((8, length), F32), vmem((n_tp - 1, 8, length), F32),
            vmem((n_tp, length, columns), F32),
            vmem((n_tp - 1, length, columns), BF16), vmem((n_tp - 1, length, columns), BF16),
            dma((9,)),
            dma((6, 2, n_sp - 1)), dma((6, 2, n_sp - 1)),
            dma((6, 2, n_sp - 1)), dma((6, 2, n_sp - 1)),
            dma((2,)), dma((2,)), dma((2,)), dma((2,)),
            dma((n_tp - 1,)), dma((n_tp - 1,)), dma((n_tp - 1,)), dma((n_tp - 1,)),
        ]
        return pl.pallas_call(
            functools.partial(kernel, (n_grp, n_sp, n_tp, float(channels * n_tp))),
            out_shape=jax.ShapeDtypeStruct((length, columns), BF16),
            in_specs=[anywhere, inside] + [anywhere] * 6 + [inside] * 6 + [anywhere] * 2,
            out_specs=inside,
            scratch_shapes=scratch,
            compiler_params=pltpu.CompilerParams(
                collective_id=0, has_side_effects=True, vmem_limit_bytes=60 * 1024 * 1024
            ),
        )(
            tokens_in, input_gain.reshape(1, width), w_key, w_gates.T, w_value, w_query,
            w_glu_value, sigmoid_opener_matrix, log_decay, log_decay.T,
            head_gain.reshape(1, head_width), conv_kernel, norm_gain.reshape(1, channels),
            norm_shift.reshape(1, channels), out_delta, out_conv,
        )

    placed = (
        P(("grp", "sp"), None), P(), P("sp", "tp"), P("sp", "tp"), P("sp", "tp"), P("sp", "tp"),
        P("sp", "tp"), P("sp", "tp"), P(("grp", "sp"), "tp"), P(), P(None, "tp"), P("tp"), P("tp"),
        P(None, "tp"), P(None, "tp"),
    )
    return jax.shard_map(
        on_device, mesh=mesh, in_specs=placed, out_specs=P(("grp", "sp"), "tp"), check_vma=False
    )
```

```python
import functools

import jax
import jax.numpy as jnp
from jax import lax
from jax.experimental import pallas as pl
from jax.experimental.pallas import tpu as pltpu
from jax.sharding import PartitionSpec as P

EPSILON = 1e-06
BETA_SHIFT = 6.0
HALO = 16
MESH = pl.DeviceIdType.MESH
F32 = jnp.float32
BF16 = jnp.bfloat16
NT = (((1,), (1,)), ((), ()))
TN = (((0,), (0,)), ((), ()))
NN = (((1,), (0,)), ((), ()))
KEY, GATE, VALUE, QUERY, GLU, OPEN = range(6)


def bdot(left, right, dims=NN):
    return lax.dot_general(
        left.astype(BF16), right.astype(BF16), dims, preferred_element_type=F32
    )


def each(count, action):
    if count <= 8:
        for step in range(count):
            action(step)
    else:
        def body(step, carry):
            action(step)
            return carry

        lax.fori_loop(0, count, body, 0)


def kernel(cfg, tok_h, gain, wk_h, wg_h, wv_h, wq_h, wa_h, wb_h, ld, ldt, hgain, ck, ng, ns, od_h, oc_h,
           out,
           tok, normed, wk, wg, wv, wq, wa, wb, od, oc,
           keys, vals, betas, cums, xinv, gaps, rhs, local_out, reads, maps, ends,
           chain_in, chain_out, glu, halo, pad, conv, stat_out, stat_in, conv_acc, part_out, part_in, pair_out, pair_in,
           local_sem, z_send, z_recv, y_send, y_recv, chain_send, chain_recv,
           halo_send, halo_recv, stat_send, stat_recv, part_send, part_recv, pair_send, pair_recv):
    n_grp, n_sp, n_tp, conv_total = cfg
    grp, sp, tp = lax.axis_index("grp"), lax.axis_index("sp"), lax.axis_index("tp")
    length, width = tok.shape
    rows = wk_h.shape[0]
    channels = wa.shape[1]
    head_width = hgain.shape[1]
    heads = wk.shape[1] // head_width
    share = (rows // 2) // 16 * 16 if n_grp == 2 else 0
    pulled = rows - share

    sources = (wk_h, wg_h, wv_h, wq_h, wa_h, wb_h)
    targets = (wk, wg, wv, wq, wa, wb)

    def block_of(w, index, start, count):
        if w == GATE:
            return targets[w].at[index]
        return targets[w].at[pl.ds(pl.multiple_of(index * rows + start, 16), count)]

    load_tok = pltpu.make_async_copy(tok_h, tok, local_sem.at[0])
    load_tok.start()
    own = [
        pltpu.make_async_copy(sources[w], block_of(w, sp, 0, rows), local_sem.at[1 + w])
        for w in range(6)
    ]
    for copy in own:
        copy.start()
    load_od = pltpu.make_async_copy(od_h, od, local_sem.at[7])
    load_oc = pltpu.make_async_copy(oc_h, oc, local_sem.at[8])

    barrier = pltpu.get_barrier_semaphore()

    def greet(axis, me, count):
        def one(step):
            pl.semaphore_signal(
                barrier, inc=1, device_id={axis: lax.rem(me + step + 1, count)}, device_id_type=MESH
            )

        each(count - 1, one)

    greet("sp", sp, n_sp)
    greet("tp", tp, n_tp)
    greet("grp", grp, n_grp)
    pl.semaphore_wait(barrier, n_sp + n_tp + n_grp - 3)

    def origin(side, d):
        return sp - d if side == 0 else sp + d

    def arrives(side, d):
        return sp - d >= 0 if side == 0 else sp + d < n_sp

    def leaves(side, d):
        if side == 0:
            return (sp - (d - 1) >= 0) & (sp < n_sp - 1)
        return (sp + (d - 1) < n_sp) & (sp > 0)

    def part_of(w, index, side_of):
        if w == GATE:
            return block_of(w, index, 0, 0)
        if not share:
            return block_of(w, index, 0, rows)
        if side_of is None:
            return block_of(w, index, pl.multiple_of(grp * share, 16), pulled)
        return block_of(w, index, pl.multiple_of(side_of * pulled, 16), share)

    def z_copy(w, side, d, first=False):
        target = part_of(w, origin(side, d - 1), None)
        source = target
        if first:
            source = sources[w]
            if w != GATE and share:
                source = source.at[pl.ds(pl.multiple_of(grp * share, 16), pulled)]
        return pltpu.make_async_remote_copy(
            src_ref=source, dst_ref=target,
            send_sem=z_send.at[w, side, d - 1], recv_sem=z_recv.at[w, side, d - 1],
            device_id={"sp": sp + 1 if side == 0 else sp - 1}, device_id_type=MESH,
        )

    def z_arrival(w, side, d):
        place = part_of(w, origin(side, d), None)
        return pltpu.make_async_remote_copy(
            src_ref=place, dst_ref=place,
            send_sem=z_send.at[w, side, d - 1], recv_sem=z_recv.at[w, side, d - 1],
            device_id={"sp": sp + 1 if side == 0 else sp - 1}, device_id_type=MESH,
        )

    def y_copy(w, side, d, arriving=False):
        place = part_of(w, origin(side, d), 1 - grp if arriving else grp)
        return pltpu.make_async_remote_copy(
            src_ref=place, dst_ref=place,
            send_sem=y_send.at[w, side, d - 1], recv_sem=y_recv.at[w, side, d - 1],
            device_id={"grp": 1 - grp}, device_id_type=MESH,
        )

    def offer(w):
        for side in range(2):
            @pl.when(leaves(side, 1))
            def _(side=side):
                z_copy(w, side, 1, True).start()

    def relay_hop(w, d):
        for side in range(2):
            @pl.when(arrives(side, d))
            def _(side=side):
                z_arrival(w, side, d).wait_recv()

                @pl.when(leaves(side, d + 1))
                def _():
                    z_copy(w, side, d + 1).start()

                if share and w != GATE:
                    y_copy(w, side, d).start()

    def relay(w, low=1, high=None):
        if high is None:
            each(n_sp - low, lambda step: relay_hop(w, step + low))
        else:
            for d in range(low, min(high, n_sp - 1) + 1):
                relay_hop(w, d)

    def complete(w):
        own[w].wait()
        if share and w != GATE:
            def one(step):
                for side in range(2):
                    @pl.when(arrives(side, step + 1))
                    def _(side=side):
                        y_copy(w, side, step + 1, True).wait_recv()

            each(n_sp - 1, one)

    offer(KEY)
    offer(GATE)
    offer(VALUE)
    load_od.start()
    load_oc.start()

    load_tok.wait()
    chunk = 64
    for at in range(0, length, chunk):
        here = tok[at:at + chunk, :].astype(F32)
        scale = lax.rsqrt(jnp.mean(here * here, axis=-1, keepdims=True) + EPSILON)
        normed[at:at + chunk, :] = (here * scale * gain[...]).astype(BF16)

    def project(w):
        return jnp.dot(normed[...], targets[w][...], preferred_element_type=F32)

    def unit_rows(tensor):
        return tensor * lax.rsqrt(jnp.sum(tensor * tensor, axis=-1, keepdims=True) + EPSILON)

    def silu(tensor):
        return tensor * jax.nn.sigmoid(tensor)

    relay(GATE)
    relay(KEY)
    offer(QUERY)
    complete(GATE)
    gate_cols = jnp.zeros((length, 4 * heads), F32)
    gate_rows = jnp.zeros((4 * heads, length), F32)
    for index in range(n_sp):
        normed_part = normed[:, index * rows:(index + 1) * rows]
        gate_cols = gate_cols + lax.dot_general(normed_part, wg[index], NT, preferred_element_type=F32)
        gate_rows = gate_rows + lax.dot_general(wg[index], normed_part, NT, preferred_element_type=F32)

    row_at = lax.broadcasted_iota(jnp.int32, (length, length), 0)
    col_at = lax.broadcasted_iota(jnp.int32, (length, length), 1)

    complete(KEY)
    key_proj = silu(project(KEY))
    pairs = [(h, r) for h in range(heads) for r in range(2)]
    for h in range(heads):
        keys[h] = unit_rows(key_proj[:, h * head_width:(h + 1) * head_width])
    relay(VALUE, 1, 1)
    for h in range(heads):
        grams = bdot(keys[h], keys[h], NT)
        for r in range(2):
            p = 2 * h + r
            decay_col = ld[:, p:p + 1] * (0.5 + jax.nn.sigmoid(gate_cols[:, 2 * p:2 * p + 1]))
            decay_row = ldt[p:p + 1, :] * (0.5 + jax.nn.sigmoid(gate_rows[2 * p:2 * p + 1, :]))
            beta = jax.nn.sigmoid(gate_cols[:, 2 * p + 1:2 * p + 2] - BETA_SHIFT)
            if r == 0:
                seen_down, seen_across = row_at <= col_at, col_at <= row_at
            else:
                seen_down, seen_across = row_at >= col_at, col_at >= row_at
            cum_row = jnp.sum(jnp.where(seen_down, decay_col, 0.0), axis=0, keepdims=True)
            cum_col = jnp.sum(jnp.where(seen_across, decay_row, 0.0), axis=1, keepdims=True)
            weighting = jnp.where(
                seen_across, jnp.exp(jnp.where(seen_across, cum_col - cum_row, 0.0)), 0.0
            )
            gaps[p] = weighting
            betas[p] = jnp.broadcast_to(beta, (length, head_width))
            cums[p] = jnp.broadcast_to(cum_col, (length, head_width))
            lower = jnp.where(row_at != col_at, grams * weighting * beta, 0.0)
            rhs[p] = lower
            near = (row_at // 2 == col_at // 2)
            xinv[p] = jnp.where(row_at == col_at, 1.0, jnp.where(near, -lower, 0.0))

    size = 2
    while size < length:
        inside = (row_at // (2 * size) == col_at // (2 * size)) & (row_at // size != col_at // size)
        for p in range(len(pairs)):
            across = jnp.where(inside, rhs[p], 0.0)
            inverse = xinv[p]
            xinv[p] = inverse - bdot(inverse, bdot(across, inverse))
        if size == 2:
            relay(VALUE, 2)
            offer(GLU)
        if size == 32:
            relay(QUERY, 1, 1)
        if size == 128:
            relay(QUERY, 2, 2)
        size *= 2

    complete(VALUE)
    value_proj = silu(project(VALUE))
    eye = (
        lax.broadcasted_iota(jnp.int32, (head_width, head_width), 0)
        == lax.broadcasted_iota(jnp.int32, (head_width, head_width), 1)
    )
    for h, r in pairs:
        p = 2 * h + r
        beta, cum, key = betas[p], cums[p], keys[h]
        value = value_proj[:, h * head_width:(h + 1) * head_width]
        total = cum[length - 1:length, :] if r == 0 else cum[0:1, :]
        right = jnp.concatenate([beta * value, beta * key * jnp.exp(cum)], axis=1)
        solved = bdot(xinv[p], right)
        vals[p] = solved.astype(BF16)
        passed = bdot(key * jnp.exp(total - cum), solved, TN)
        ends[p] = passed[:, :head_width]
        maps[p] = (jnp.where(eye, jnp.exp(total), 0.0) - passed[:, head_width:]).astype(BF16)

    def place_of(r):
        return sp if r == 0 else n_sp - 1 - sp

    def chain_copy(r):
        dest = lax.rem(sp + 1, n_sp) if r == 0 else lax.rem(sp + n_sp - 1, n_sp)
        return pltpu.make_async_remote_copy(
            src_ref=chain_out.at[r], dst_ref=chain_in.at[r],
            send_sem=chain_send.at[r], recv_sem=chain_recv.at[r],
            device_id={"sp": dest}, device_id_type=MESH,
        )

    def chain_point(low, high):
        for r in range(2):
            at = place_of(r)

            @pl.when((at >= low) & (at <= high))
            def _(r=r, at=at):
                if low == 0:
                    for h in range(heads):
                        chain_in[r, h] = jnp.zeros((head_width, head_width), BF16)
                        chain_out[r, h] = ends[2 * h + r].astype(BF16)
                else:
                    chain_copy(r).wait_recv()
                    for h in range(heads):
                        p = 2 * h + r
                        chain_out[r, h] = (bdot(maps[p], chain_in[r, h]) + ends[p]).astype(BF16)

                @pl.when(at < n_sp - 1)
                def _():
                    chain_copy(r).start()

    chain_point(0, 0)
    relay(QUERY, 3)
    offer(OPEN)
    relay(GLU, 1, 1)
    complete(QUERY)
    query_proj = silu(project(QUERY))
    for h in range(heads):
        query = unit_rows(query_proj[:, h * head_width:(h + 1) * head_width]) * head_width ** -0.5
        scores = bdot(query, keys[h], NT)
        for r in range(2):
            p = 2 * h + r
            both = jnp.dot((scores * gaps[p]).astype(BF16), vals[p], preferred_element_type=F32)
            reads[p] = (query * jnp.exp(cums[p]) - both[:, head_width:]).astype(BF16)
            if r == 0:
                local_out[h] = both[:, :head_width]
            else:
                local_out[h] = local_out[h] + both[:, :head_width]
    chain_point(1, 1)
    relay(GLU, 2, 2)
    chain_point(2, 2)
    relay(GLU, 3)
    relay(OPEN, 1, 1)
    chain_point(3, n_sp - 1)
    complete(GLU)
    glu_proj = project(GLU)
    relay(OPEN, 2)
    complete(OPEN)
    gated = (glu_proj * jax.nn.sigmoid(project(OPEN))).astype(BF16)
    glu[...] = gated
    pad[HALO:HALO + length, :] = gated.astype(F32)

    def halo_copy(r):
        start = length - HALO if r == 0 else 0
        dest = lax.rem(sp + 1, n_sp) if r == 0 else lax.rem(sp + n_sp - 1, n_sp)
        return pltpu.make_async_remote_copy(
            src_ref=glu.at[pl.ds(start, HALO)], dst_ref=halo.at[r],
            send_sem=halo_send.at[r], recv_sem=halo_recv.at[r],
            device_id={"sp": dest}, device_id_type=MESH,
        )

    for r in range(2):
        @pl.when(place_of(r) < n_sp - 1)
        def _(r=r):
            halo_copy(r).start()
    for r in range(2):
        start = 0 if r == 0 else HALO + length

        @pl.when(place_of(r) > 0)
        def _(r=r, start=start):
            halo_copy(r).wait_recv()
            pad[start:start + HALO, :] = halo[r].astype(F32)

        @pl.when(place_of(r) == 0)
        def _(start=start):
            pad[start:start + HALO, :] = jnp.zeros((HALO, channels), F32)

    taps = ck.shape[0]
    for at in range(0, length, chunk):
        first = at + HALO - taps // 2
        total = pad[first:first + chunk, :] * ck[0:1, :]
        for j in range(1, taps):
            total = total + pad[first + j:first + j + chunk, :] * ck[j:j + 1, :]
        conv[at:at + chunk, :] = total
    filtered = conv[...]
    sum_col = jnp.sum(filtered, axis=-1, keepdims=True)
    square_col = jnp.sum(filtered * filtered, axis=-1, keepdims=True)
    same = row_at == col_at
    stat_out[...] = jnp.zeros(stat_out.shape, F32)
    stat_out[0:1, :] = jnp.sum(jnp.where(same, sum_col, 0.0), axis=0, keepdims=True)
    stat_out[1:2, :] = jnp.sum(jnp.where(same, square_col, 0.0), axis=0, keepdims=True)

    def stat_copy(step):
        return pltpu.make_async_remote_copy(
            src_ref=stat_out, dst_ref=stat_in.at[step],
            send_sem=stat_send.at[step], recv_sem=stat_recv.at[step],
            device_id={"tp": lax.rem(tp + step + 1, n_tp)}, device_id_type=MESH,
        )

    for step in range(n_tp - 1):
        stat_copy(step).start()

    joined_heads = []
    for h in range(heads):
        joined = local_out[h] + jnp.dot(reads[2 * h], chain_in[0, h], preferred_element_type=F32)
        joined = joined + jnp.dot(reads[2 * h + 1], chain_in[1, h], preferred_element_type=F32)
        scale = lax.rsqrt(jnp.mean(joined * joined, axis=-1, keepdims=True) + EPSILON)
        joined_heads.append((joined * scale * hgain[...]).astype(BF16))
    delta_mix = jnp.concatenate(joined_heads, axis=1) if heads > 1 else joined_heads[0]
    load_od.wait()
    load_oc.wait()
    columns = width // n_tp
    for dest in range(n_tp):
        at = slice(dest * columns, (dest + 1) * columns)
        conv_acc[dest] = lax.dot_general(delta_mix, od[at, :], NT, preferred_element_type=F32)

    stats = stat_out[0:2, :]
    for step in range(n_tp - 1):
        stat_copy(step).wait_recv()
        stats = stats + stat_in[step, 0:2, :]
    center = jnp.sum(jnp.where(same, stats[0:1, :], 0.0), axis=1, keepdims=True) / conv_total
    squares = jnp.sum(jnp.where(same, stats[1:2, :], 0.0), axis=1, keepdims=True) / conv_total
    spread = squares - center * center
    normal = (filtered - center) * lax.rsqrt(spread + EPSILON)
    conv_mix = silu(normal * ng[...] + ns[...]).astype(BF16)

    chip, core = tp // 2, lax.rem(tp, 2)
    chips = n_tp // 2
    sibling = chip * 2 + 1 - core

    def there(p, place):
        return lax.rem(chip + p, chips) * 2 + place

    def term_of(dest):
        at = pl.ds(pl.multiple_of(dest * columns, 16), columns)
        return conv_acc[dest] + lax.dot_general(conv_mix, oc[at, :], NT, preferred_element_type=F32)

    def pair_copy(p):
        return pltpu.make_async_remote_copy(
            src_ref=pair_out.at[p], dst_ref=pair_in.at[p],
            send_sem=pair_send.at[p], recv_sem=pair_recv.at[p],
            device_id={"tp": sibling}, device_id_type=MESH,
        )

    def part_copy(p):
        return pltpu.make_async_remote_copy(
            src_ref=part_out.at[p - 1], dst_ref=part_in.at[p - 1],
            send_sem=part_send.at[p - 1], recv_sem=part_recv.at[p - 1],
            device_id={"tp": there(p, core)}, device_id_type=MESH,
        )

    slots = list(range(1, chips)) + [0]
    for p in slots:
        pair_out[p] = term_of(there(p, 1 - core)).astype(BF16)
        pair_copy(p).start()
    for p in slots:
        term = term_of(there(p, core))
        pair_copy(p).wait_recv()
        term = term + pair_in[p].astype(F32)
        if p:
            part_out[p - 1] = term.astype(BF16)
            part_copy(p).start()
        else:
            result = term
    for p in range(1, chips):
        part_copy(p).wait_recv()
        result = result + part_in[p - 1].astype(F32)
    out[...] = result.astype(BF16)

    for w in range(6):
        def one(step, w=w):
            for side in range(2):
                @pl.when(leaves(side, step + 1))
                def _(side=side):
                    z_copy(w, side, step + 1).wait_send()

                if share and w != GATE:
                    @pl.when(arrives(side, step + 1))
                    def _(side=side):
                        y_copy(w, side, step + 1).wait_send()

        each(n_sp - 1, one)
    for r in range(2):
        @pl.when(place_of(r) < n_sp - 1)
        def _(r=r):
            chain_copy(r).wait_send()
            halo_copy(r).wait_send()
    for step in range(n_tp - 1):
        stat_copy(step).wait_send()
    for p in range(chips):
        pair_copy(p).wait_send()
        if p:
            part_copy(p).wait_send()


def solution(mesh):
    n_grp, n_sp, n_tp = mesh.shape["grp"], mesh.shape["sp"], mesh.shape["tp"]

    def on_device(tokens_in, input_gain, w_query, w_key, w_value, w_gates, w_glu_value,
                  sigmoid_opener_matrix, log_decay, head_gain, conv_kernel, norm_gain, norm_shift,
                  out_delta, out_conv):
        length, width = tokens_in.shape
        head_width = head_gain.shape[0]
        head_cols = w_query.shape[1]
        heads = head_cols // head_width
        channels = w_glu_value.shape[1]
        rows = w_query.shape[0]
        pairs = 2 * heads
        columns = width // n_tp
        dma, vmem = pltpu.SemaphoreType.DMA, pltpu.VMEM
        anywhere = pl.BlockSpec(memory_space=pltpu.HBM)
        inside = pl.BlockSpec(memory_space=pltpu.VMEM)
        scratch = [
            vmem((length, width), BF16), vmem((length, width), BF16),
            vmem((width, head_cols), BF16), vmem((n_sp, 4 * heads, rows), BF16),
            vmem((width, head_cols), BF16), vmem((width, head_cols), BF16),
            vmem((width, channels), BF16), vmem((width, channels), BF16),
            vmem((width, head_cols), BF16), vmem((width, channels), BF16),
            vmem((heads, length, head_width), F32), vmem((pairs, length, 2 * head_width), BF16),
            vmem((pairs, length, head_width), F32), vmem((pairs, length, head_width), F32),
            vmem((pairs, length, length), F32), vmem((pairs, length, length), F32),
            vmem((pairs, length, length), F32),
            vmem((heads, length, head_width), F32), vmem((pairs, length, head_width), BF16),
            vmem((pairs, head_width, head_width), BF16), vmem((pairs, head_width, head_width), F32),
            vmem((2, heads, head_width, head_width), BF16), vmem((2, heads, head_width, head_width), BF16),
            vmem((length, channels), BF16), vmem((2, HALO, channels), BF16),
            vmem((length + 2 * HALO, channels), F32), vmem((length, channels), F32),
            vmem((8, length), F32), vmem((n_tp - 1, 8, length), F32),
            vmem((n_tp, length, columns), F32),
            vmem((n_tp // 2, length, columns), BF16), vmem((n_tp // 2, length, columns), BF16),
            vmem((n_tp // 2, length, columns), BF16), vmem((n_tp // 2, length, columns), BF16),
            dma((9,)),
            dma((6, 2, n_sp - 1)), dma((6, 2, n_sp - 1)),
            dma((6, 2, n_sp - 1)), dma((6, 2, n_sp - 1)),
            dma((2,)), dma((2,)), dma((2,)), dma((2,)),
            dma((n_tp - 1,)), dma((n_tp - 1,)), dma((n_tp // 2,)), dma((n_tp // 2,)),
            dma((n_tp // 2,)), dma((n_tp // 2,)),
        ]
        return pl.pallas_call(
            functools.partial(kernel, (n_grp, n_sp, n_tp, float(channels * n_tp))),
            out_shape=jax.ShapeDtypeStruct((length, columns), BF16),
            in_specs=[anywhere, inside] + [anywhere] * 6 + [inside] * 6 + [anywhere] * 2,
            out_specs=inside,
            scratch_shapes=scratch,
            compiler_params=pltpu.CompilerParams(
                collective_id=0, has_side_effects=True, vmem_limit_bytes=60 * 1024 * 1024
            ),
        )(
            tokens_in, input_gain.reshape(1, width), w_key, w_gates.T, w_value, w_query,
            w_glu_value, sigmoid_opener_matrix, log_decay, log_decay.T,
            head_gain.reshape(1, head_width), conv_kernel, norm_gain.reshape(1, channels),
            norm_shift.reshape(1, channels), out_delta, out_conv,
        )

    placed = (
        P(("grp", "sp"), None), P(), P("sp", "tp"), P("sp", "tp"), P("sp", "tp"), P("sp", "tp"),
        P("sp", "tp"), P("sp", "tp"), P(("grp", "sp"), "tp"), P(), P(None, "tp"), P("tp"), P("tp"),
        P(None, "tp"), P(None, "tp"),
    )
    return jax.shard_map(
        on_device, mesh=mesh, in_specs=placed, out_specs=P(("grp", "sp"), "tp"), check_vma=False
    )
```
